32 devices in a mesh: ep: 16 (over z, y, x), tp: 2 (over core).
Axes of the slice: x: 2, y: 2, z: 4, core: 2. Of those that a mesh axis runs over, the one named last changes fastest.
Arguments:
- residual: bfloat16 [1024, 2048], P('ep', 'tp'), may hold values from -100 to 100
- route_ids: int32 [1024, 4], P('ep'), may hold values from 0 to 15, all different within a row; in each aligned block of 64 rows (0 to 63, 64 to 127, ...) at most 24 rows name the same one
- route_weights: float32 [1024, 4], P('ep'), may hold values from 0.1 to 1
- carried_state: float32 [2, 1024, 4096], P(None, 'ep', 'tp'), may hold values from -6 to 6
- mix_gain: float32 [2048], replicated, may hold values from 0.1 to 1.9
- in_proj: bfloat16 [2048, 1024], P(None, 'tp'), may hold values from -0.125 to 0.125
- decay_rate: float32 [64, 64], P('tp'), may hold values from 0.1 to 2
- frequency: float32 [64, 64], P('tp'), may hold values from -3 to 3
- step_size: float32 [64], P('tp'), may hold values from 0.05 to 1
- input_map: float32 [2, 64, 64, 16], P(None, 'tp'), may hold values from -1.5 to 1.5
- output_matrix: float32 [2, 64, 16, 64], P(None, 'tp'), may hold values from -0.5 to 0.5
- passthrough_scale: float32 [1024], P('tp'), may hold values from -4 to 4
- out_gain: float32 [1024], replicated, may hold values from 0.1 to 1.9
- out_proj: bfloat16 [1024, 2048], P(None, 'tp'), may hold values from -0.1875 to 0.1875
- ffn_gain: float32 [2048], replicated, may hold values from 0.1 to 1.9
- w_gate: bfloat16 [16, 2048, 2048], P('ep', None, 'tp'), may hold values from -5 to 5
- w_up: bfloat16 [16, 2048, 2048], P('ep', None, 'tp'), may hold values from -5 to 5
- w_down: bfloat16 [16, 2048, 2048], P('ep', 'tp'), may hold values from -0.125 to 0.125
Outputs:
- updated: bfloat16 [1024, 2048], P('ep', 'tp')
- new_state: float32 [2, 1024, 4096], P(None, 'ep', 'tp')
The draws below stay inside these ranges and needn't reach their ends.
Inputs may be any that keep to these rules, and one draw needn't show every extreme that they name: `route_ids`: each row names 4 different experts. Among the 64 rows of one device (aligned blocks) no expert is named more than 24 times, and in every draw some block names some expert exactly 24 times.
All inputs are finite; a program needn't handle non-finite values.
Results may differ from the reference program's by a relative error of at most 0.018.
Values may be sent and summed in bfloat16 or wider, within the bound.
No kernel may reach another device: no remote copies, remote signals or barrier semaphores. Data moves between devices by JAX's collectives and lax.ppermute only.
A program may use at most 128 MiB of HBM per device.

```python
import math
import jax
import jax.numpy as jnp
import numpy as np
from jax import lax

D = 2048
S5W = 1024
GROUP_CH = 16
GROUPS = 64
STATE = 64
FF = 2048
EXPERTS = 16
TOPK = 4
SEQ_DEV = 64
TOKENS = 1024
CAP = 24
WIDTH_SPLIT = 2
N_EP = 16


def draw_residual(key, part):
    key_one = jax.random.fold_in(key, 11)
    key_three = jax.random.fold_in(key, 13)
    column_pos = jnp.arange(D, dtype=jnp.float32) / D
    column_ramp = jnp.exp(math.log(3.0) * column_pos)
    base_draw = jnp.clip(jax.random.normal(key_one, (TOKENS, D), jnp.float32), -5.0, 5.0)
    jitter = jnp.exp(jax.random.uniform(key_three, (1, D), jnp.float32, -0.35, 0.35))
    return (base_draw * column_ramp * jitter / 1.5).astype(jnp.bfloat16)


def expert_weight(key, salt_value):
    key_one = jax.random.fold_in(key, salt_value)
    key_two = jax.random.fold_in(key, salt_value + 1)
    base_draw = jnp.clip(jax.random.normal(key_one, (EXPERTS, D, FF), jnp.float32), -5.0, 5.0) / math.sqrt(D)
    top_scale = 3.0
    column_scale = 0.5 * jnp.exp(jax.random.uniform(key_two, (EXPERTS, 1, FF), jnp.float32, 0.0, math.log(top_scale / 0.5)))
    return (base_draw * column_scale).astype(jnp.bfloat16)


def draw_w_gate(key, part):
    return expert_weight(key, 21)


def draw_w_up(key, part):
    return expert_weight(key, 31)


def block_levels(stream_key, dims, split, smallest, largest):
    factor_of = 1.0
    for axis_at, shards_of in split:
        heights = jax.random.uniform(jax.random.fold_in(jax.random.fold_in(stream_key, 6), axis_at), (shards_of,), jnp.float32, smallest / len(split), largest / len(split))
        factor_of = factor_of * jnp.repeat(jnp.exp(heights), dims[axis_at] // shards_of).reshape((-1,) + (1,) * (len(dims) - 1 - axis_at))
    return factor_of


def deal_out(own_key, own, number, rows, count, top, limit, lean):
    ranking = jax.random.permutation(own_key, count)
    packed, common = load_shares(count, rows * top, limit, lean, True), load_shares(count, rows * top, limit, lean, False)
    places = jnp.arange(count)

    def named(tallies, turn):
        used = int((tallies > 0).sum())
        fixed = max(1, used // 4)
        moved = fixed + (places - fixed + turn * (used - fixed)) % max(1, count - fixed)
        return jnp.zeros((count,), jnp.int32).at[ranking[jnp.where(places < fixed, places, moved)]].set(jnp.asarray(tallies, jnp.int32))

    tallies = jnp.where(number % 4 == 0, named(packed, number // 4), named(common, number - number // 4 - 1))
    mixed = jax.random.permutation(jax.random.fold_in(own, 3), count)
    source_of, taker = mixed[0:count // 2 * 2:2], mixed[1:count // 2 * 2:2]
    slack = jnp.minimum(tallies[source_of] - 1, limit - tallies[taker]) // 2
    slack = jnp.where((source_of == ranking[0]) | (taker == ranking[0]) | (tallies[taker] == 0), 0, jnp.maximum(slack, 0))
    moved = jax.random.randint(jax.random.fold_in(own, 4), (count // 2,), 0, 1 << 20) % (slack + 1)
    tallies = tallies.at[source_of].add(-moved).at[taker].add(moved)
    labels = jnp.searchsorted(jnp.cumsum(tallies), jnp.arange(rows * top), side="right").astype(jnp.int32)
    grid = labels.reshape(top, rows).T
    grid = grid[jax.random.permutation(jax.random.fold_in(own, 1), rows)]
    turn = jax.random.randint(jax.random.fold_in(own, 2), (rows, 1), 0, top)
    return jnp.take_along_axis(grid, (jnp.arange(top)[None, :] + turn) % top, axis=1)


def load_shares(count, total, bound, slope, full):
    portions = [(1 << 20) // math.isqrt(grade ** slope) + 1 for grade in range(1, count + 1)]
    largest = bound if full else min(bound, max(-(-total // count), total * portions[0] // sum(portions)))
    least = 1 if total - largest >= count - 1 else 0
    counts, surplus = [largest] + [least] * (count - 1), total - largest - least * (count - 1)
    while surplus > 0:
        free = [i for i in range(1, count) if counts[i] < largest] or [i for i in range(1, count) if counts[i] < bound]
        pool, left = sum([portions[i] for i in free]), surplus
        for i in free:
            addition = min(bound - counts[i], max(1, left * portions[i] // pool), surplus)
            counts[i] = counts[i] + addition
            surplus = surplus - addition
    return np.array(counts)


def scatter_about(own_key, shape, scale, bound, cuts=(), kind=jnp.bfloat16):
    factor_of = block_levels(own_key, shape, cuts, -0.22, 0.18) if cuts else 1.0
    entries = jax.random.normal(own_key, shape, jnp.float32) * scale * factor_of
    return jnp.minimum(jnp.maximum(entries, -bound), bound).astype(kind)


def setup_inputs(seed: int = 0) -> dict:
    arg_keys = jax.random.split(jax.random.key(seed), 19)
    residual = draw_residual(jax.random.fold_in(arg_keys[18], 71), 0)
    route_ids_keys = jax.random.split(jax.random.fold_in(arg_keys[1], 1), TOKENS // SEQ_DEV)
    route_ids_turns = jax.random.permutation(jax.random.fold_in(arg_keys[1], 3), TOKENS // SEQ_DEV)
    route_ids = jax.vmap(lambda own, number: deal_out(jax.random.fold_in(arg_keys[1], 2), own, number, SEQ_DEV, EXPERTS, TOPK, CAP, 1))(route_ids_keys, route_ids_turns).reshape((TOKENS, TOPK))
    route_weights = jnp.clip(0.1 + 0.9 * jax.random.uniform(arg_keys[2], (TOKENS, TOPK), jnp.float32) ** block_levels(arg_keys[2], (TOKENS, TOPK), ((0, 16),), -0.2, 0.2), 0.1, 1.0)
    carried_state = scatter_about(arg_keys[3], (2, TOKENS, GROUPS * STATE), 1.0, 6.0, ((1, 16), (2, 2)), jnp.float32)
    mix_gain = jnp.clip(1.0 + 0.18 * jax.random.normal(arg_keys[4], (D,), jnp.float32), 0.1, 1.9)
    in_proj = scatter_about(arg_keys[5], (D, S5W), D ** -0.5, 0.125, ((1, 2),))
    decay_rate = jnp.clip(jnp.exp(math.log(2.0) - 2.9957323 * jax.random.uniform(arg_keys[6], (GROUPS, STATE), jnp.float32) ** block_levels(arg_keys[6], (GROUPS, STATE), ((0, 2),), -0.2, 0.2)), 0.1, 2.0)
    frequency = jnp.clip(jax.random.uniform(arg_keys[7], (GROUPS, STATE), jnp.float32, -3.0, 3.0) * block_levels(arg_keys[7], (GROUPS, STATE), ((0, 2),), -0.4, 0.0), -3.0, 3.0)
    step_size = jnp.clip(jnp.exp(math.log(1.0) - 2.9957323 * jax.random.uniform(arg_keys[8], (GROUPS,), jnp.float32) ** block_levels(arg_keys[8], (GROUPS,), ((0, 2),), -0.2, 0.2)), 0.05, 1.0)
    input_map = scatter_about(arg_keys[9], (2, GROUPS, STATE, GROUP_CH), GROUP_CH ** -0.5, 1.5, ((1, 2),), jnp.float32)
    output_matrix = scatter_about(arg_keys[10], (2, GROUPS, GROUP_CH, STATE), (2 * STATE) ** -0.5, 0.5, ((1, 2),), jnp.float32)
    passthrough_scale = scatter_about(arg_keys[11], (S5W,), 1.0, 4.0, ((0, 2),), jnp.float32)
    out_gain = jnp.clip(1.0 + 0.18 * jax.random.normal(arg_keys[12], (S5W,), jnp.float32), 0.1, 1.9)
    out_proj = scatter_about(arg_keys[13], (S5W, D), S5W ** -0.5, 0.1875, ((1, 2),))
    ffn_gain = jnp.clip(1.0 + 0.18 * jax.random.normal(arg_keys[14], (D,), jnp.float32), 0.1, 1.9)
    w_gate = draw_w_gate(jax.random.fold_in(arg_keys[18], 71), 0)
    w_up = draw_w_up(jax.random.fold_in(arg_keys[18], 71), 0)
    w_down = scatter_about(arg_keys[17], (EXPERTS, FF, D), FF ** -0.5, 0.125, ((0, 16), (1, 2)))
    return {"residual": residual, "route_ids": route_ids, "route_weights": route_weights, "carried_state": carried_state, "mix_gain": mix_gain, "in_proj": in_proj, "decay_rate": decay_rate, "frequency": frequency, "step_size": step_size, "input_map": input_map, "output_matrix": output_matrix, "passthrough_scale": passthrough_scale, "out_gain": out_gain, "out_proj": out_proj, "ffn_gain": ffn_gain, "w_gate": w_gate, "w_up": w_up, "w_down": w_down}


epsilon = 1e-06
clamp_limit = 7.0
swish_alpha = 1.702

def rms_rows(values, gain_vec):
    return values * lax.rsqrt(lax.optimization_barrier(jnp.mean(values * values, axis=1, keepdims=True)) + epsilon) * gain_vec

def discretize(decay_rate, frequency, step_size):
    rate_real = -decay_rate
    rate_imag = frequency
    time_step = step_size[:, None]
    magnitude = jnp.exp(rate_real * time_step)
    phase_angle = rate_imag * time_step
    bar_real = magnitude * jnp.cos(phase_angle)
    bar_imag = magnitude * jnp.sin(phase_angle)
    denominator = rate_real * rate_real + rate_imag * rate_imag
    shifted = bar_real - 1.0
    coef_real = (shifted * rate_real + bar_imag * rate_imag) / denominator
    coef_imag = (bar_imag * rate_real - shifted * rate_imag) / denominator
    return (bar_real, bar_imag, coef_real, coef_imag)

def state_step(channels, carried_state, decay_rate, frequency, step_size, input_map, output_matrix, passthrough_scale):
    row_count = channels.shape[0]
    number_of_groups, state_width = decay_rate.shape
    channels_per_group = input_map.shape[3]
    bar_real, bar_imag, coef_real, coef_imag = discretize(decay_rate, frequency, step_size)
    map_real = coef_real[..., None] * input_map[0] - coef_imag[..., None] * input_map[1]
    map_imag = coef_real[..., None] * input_map[1] + coef_imag[..., None] * input_map[0]
    input_rows = channels.astype(jnp.float32).reshape(row_count, number_of_groups, channels_per_group)
    largest_precision = lax.Precision.HIGHEST
    push_real = jnp.einsum('sgc,gpc->sgp', input_rows, map_real, precision=largest_precision)
    push_imag = jnp.einsum('sgc,gpc->sgp', input_rows, map_imag, precision=largest_precision)
    old_real = carried_state[0].reshape(row_count, number_of_groups, state_width)
    old_imag = carried_state[1].reshape(row_count, number_of_groups, state_width)
    updated_real = bar_real * old_real - bar_imag * old_imag + push_real
    updated_imaginary = bar_real * old_imag + bar_imag * old_real + push_imag
    mixer_output = jnp.einsum('dfk,idk->idf', output_matrix[0], updated_real, precision=largest_precision) - jnp.einsum('dfk,idk->idf', output_matrix[1], updated_imaginary, precision=largest_precision) + passthrough_scale.reshape(number_of_groups, channels_per_group) * input_rows
    activated = jax.nn.gelu(mixer_output.reshape(row_count, number_of_groups * channels_per_group)).astype(jnp.bfloat16)
    new_state = jnp.stack([updated_real.reshape(row_count, -1), updated_imaginary.reshape(row_count, -1)])
    return (activated, new_state)

def expert_apply(expert_item):
    rows_in, gate_w, up_w, down_w = expert_item
    slot_count = rows_in.shape[0]
    gate_pre = jnp.dot(rows_in, gate_w, preferred_element_type=jnp.float32)
    up_pre = jnp.dot(rows_in, up_w, preferred_element_type=jnp.float32)
    gated = jnp.minimum(gate_pre, clamp_limit)
    activation = ((jnp.clip(up_pre, -clamp_limit, clamp_limit) + 1.0) * gated * jax.nn.sigmoid(swish_alpha * gated)).astype(jnp.bfloat16)
    block_width = FF // WIDTH_SPLIT
    pieces = jnp.einsum('mtf,tfd->mtd', activation.reshape(slot_count, WIDTH_SPLIT, block_width).astype(jnp.float32), down_w.reshape(WIDTH_SPLIT, block_width, D).astype(jnp.float32))
    pieces = lax.optimization_barrier(pieces.astype(jnp.bfloat16)).astype(jnp.float32)
    return lax.optimization_barrier(jnp.sum(pieces, axis=1)).astype(jnp.bfloat16)

def reference(residual, route_ids, route_weights, carried_state, mix_gain, in_proj, decay_rate, frequency, step_size, input_map, output_matrix, passthrough_scale, out_gain, out_proj, ffn_gain, w_gate, w_up, w_down):
    start_rows = residual.astype(jnp.float32)
    normed_rows = rms_rows(start_rows, mix_gain).astype(jnp.bfloat16)
    channels = jnp.dot(normed_rows, in_proj, preferred_element_type=jnp.float32).astype(jnp.bfloat16)
    activated, new_state = state_step(channels, carried_state, decay_rate, frequency, step_size, input_map, output_matrix, passthrough_scale)
    scaled = rms_rows(activated.astype(jnp.float32), out_gain).astype(jnp.bfloat16)
    after_mixer = (start_rows + jnp.dot(scaled, out_proj, preferred_element_type=jnp.float32)).astype(jnp.bfloat16)
    expert_in = rms_rows(after_mixer.astype(jnp.float32), ffn_gain).astype(jnp.bfloat16)
    route_count = TOKENS * TOPK
    flat_ids = route_ids.reshape(route_count).astype(jnp.int32)
    onehot = (flat_ids[:, None] == jnp.arange(EXPERTS, dtype=jnp.int32)[None, :]).astype(jnp.int32)
    blocked = onehot.reshape(N_EP, SEQ_DEV * TOPK, EXPERTS)
    before = (jnp.cumsum(blocked, axis=1).astype(jnp.int32) - blocked).reshape(route_count, EXPERTS)
    slot_index = lax.optimization_barrier(jnp.sum(before * onehot, axis=1)).astype(jnp.int32)
    route_iota = jnp.arange(route_count, dtype=jnp.int32)
    block_index = (route_iota // (SEQ_DEV * TOPK)).astype(jnp.int32)
    slot_total = N_EP * CAP
    position = (flat_ids * slot_total + block_index * CAP + slot_index).astype(jnp.int32)
    source_row = (route_iota // TOPK).astype(jnp.int32)
    row_table = jnp.full((EXPERTS * slot_total,), TOKENS, dtype=jnp.int32).at[position].set(source_row)
    padded = jnp.concatenate([expert_in, jnp.zeros((1, D), jnp.bfloat16)], axis=0)
    gathered = padded[row_table].reshape(EXPERTS, slot_total, D)
    outputs = lax.map(expert_apply, (gathered, w_gate, w_up, w_down))
    picked = outputs.reshape(EXPERTS * slot_total, D)[position].reshape(TOKENS, TOPK, D)
    expert_sum = lax.optimization_barrier(jnp.sum(route_weights[:, :, None] * picked.astype(jnp.float32), axis=1))
    updated = (after_mixer.astype(jnp.float32) + expert_sum).astype(jnp.bfloat16)
    return (updated, new_state)
```

```python
import functools

import jax
import jax.numpy as jnp
from jax import lax
from jax.experimental import pallas as pl
from jax.experimental.pallas import tpu as pltpu
from jax.sharding import PartitionSpec as P

epsilon = 1e-06
clamp_limit = 7.0
swish_alpha = 1.702
f32, bf16 = jnp.float32, jnp.bfloat16
NN = (((1,), (0,)), ((), ()))
NT = (((1,), (1,)), ((), ()))
TN = (((0,), (0,)), ((), ()))


def mm(a, b, dims=NN):
    return lax.dot_general(a, b, dims, preferred_element_type=f32)


def split(values):
    high = values.astype(bf16)
    return high, (values - high.astype(f32)).astype(bf16)


def flat_row(table):
    groups, width = table.shape
    tiled = jnp.concatenate([table] * groups, axis=1)
    lane = lax.broadcasted_iota(jnp.int32, tiled.shape, 1)
    first = lax.broadcasted_iota(jnp.int32, tiled.shape, 0) * width
    own = (lane >= first) & (lane < first + width)
    return jnp.sum(jnp.where(own, tiled, 0.0), axis=0, keepdims=True)


def spread(table, count):
    _, per_group, width = table.shape
    tiled = jnp.concatenate([table] * count, axis=2)
    lane = lax.broadcasted_iota(jnp.int32, tiled.shape, 2)
    first = lax.broadcasted_iota(jnp.int32, tiled.shape, 0) * width
    own = (lane >= first) & (lane < first + width)
    return jnp.where(own, tiled, 0.0).reshape(count * per_group, count * width)


def mixer_kernel(
    own_ref,
    other_ref,
    state_ref,
    gain_ref,
    proj_ref,
    decay_ref,
    freq_ref,
    step_ref,
    map_ref,
    out_ref,
    skip_ref,
    act_ref,
    new_ref,
):
    first = lax.axis_index("tp") == 0
    own, other = own_ref[...].astype(f32), other_ref[...].astype(f32)
    half = own.shape[1]
    low, high = jnp.where(first, own, other), jnp.where(first, other, own)
    total = jnp.sum(low * low, axis=1, keepdims=True) + jnp.sum(high * high, axis=1, keepdims=True)
    scale = lax.rsqrt(total / (2 * half) + epsilon)
    gain = gain_ref[...]
    low = (low * scale * gain[:, :half]).astype(bf16)
    high = (high * scale * gain[:, half:]).astype(bf16)
    channels = (mm(low, proj_ref[:half, :]) + mm(high, proj_ref[half:, :])).astype(bf16)

    groups, width = decay_ref.shape
    per_group = map_ref.shape[2]
    step = step_ref[...]
    square = jnp.broadcast_to(step, (groups, groups))
    diagonal = lax.broadcasted_iota(jnp.int32, square.shape, 0) == lax.broadcasted_iota(
        jnp.int32, square.shape, 1
    )
    step = jnp.sum(jnp.where(diagonal, square, 0.0), axis=1, keepdims=True)
    rate, freq = -decay_ref[...], freq_ref[...]
    magnitude = jnp.exp(rate * step)
    phase = freq * step
    bar_real, bar_imag = magnitude * jnp.cos(phase), magnitude * jnp.sin(phase)
    inverse = 1.0 / (rate * rate + freq * freq)
    shifted = bar_real - 1.0
    coef_real = ((shifted * rate + bar_imag * freq) * inverse)[:, None, :]
    coef_imag = ((bar_imag * rate - shifted * freq) * inverse)[:, None, :]
    map_real = coef_real * map_ref[0] - coef_imag * map_ref[1]
    map_imag = coef_real * map_ref[1] + coef_imag * map_ref[0]
    bar_real, bar_imag = flat_row(bar_real), flat_row(bar_imag)

    count = max(1, min(groups, 128 // per_group))
    lanes, columns = count * width, count * per_group
    for block in range(groups // count):
        held = slice(block * count, (block + 1) * count)
        wide = slice(block * lanes, (block + 1) * lanes)
        narrow = slice(block * columns, (block + 1) * columns)
        fed = channels[:, narrow]
        real_high, real_low = split(spread(map_real[held], count))
        imag_high, imag_low = split(spread(map_imag[held], count))
        old_real, old_imag = state_ref[0, :, wide], state_ref[1, :, wide]
        turn_real, turn_imag = bar_real[:, wide], bar_imag[:, wide]
        next_real = (
            turn_real * old_real - turn_imag * old_imag + (mm(fed, real_high) + mm(fed, real_low))
        )
        next_imag = (
            turn_real * old_imag + turn_imag * old_real + (mm(fed, imag_high) + mm(fed, imag_low))
        )
        new_ref[0, :, wide] = next_real
        new_ref[1, :, wide] = next_imag
        a_high, a_low = split(spread(out_ref[0, held], count))
        b_high, b_low = split(spread(-out_ref[1, held], count))
        r_high, r_low = split(next_real)
        i_high, i_low = split(next_imag)
        mixed = (mm(r_high, a_high, NT) + mm(i_high, b_high, NT)) + (
            mm(r_low, a_high, NT)
            + mm(r_high, a_low, NT)
            + mm(i_low, b_high, NT)
            + mm(i_high, b_low, NT)
        )
        mixed = mixed + skip_ref[:, narrow] * fed.astype(f32)
        act_ref[:, narrow] = jax.nn.gelu(mixed).astype(bf16)


def slots_of(ids, experts, capacity):
    rows = ids.shape[1]
    expert = lax.broadcasted_iota(jnp.int32, (experts, rows), 0)
    named = jnp.zeros((experts, rows), f32)
    for k in range(ids.shape[0]):
        named = named + (ids[k : k + 1, :] == expert).astype(f32)
    earlier = lax.broadcasted_iota(jnp.int32, (rows, rows), 0) < lax.broadcasted_iota(
        jnp.int32, (rows, rows), 1
    )
    rank = mm(named.astype(bf16), earlier.astype(f32).astype(bf16))
    rank = jnp.where(named > 0.0, rank, -1.0).astype(jnp.int32)
    slot = lax.broadcasted_iota(jnp.int32, (experts, capacity, rows), 1)
    return rank[:, None, :] == slot


def dispatch_kernel(capacity, experts, own_ref, other_ref, gain_ref, proj_ref, residual_ref, ids_ref, mid_ref, sent_ref):
    first = lax.axis_index("tp") == 0
    own, other = own_ref[...].astype(f32), other_ref[...].astype(f32)
    half = own.shape[1]
    low, high = jnp.where(first, own, other), jnp.where(first, other, own)
    total = jnp.sum(low * low, axis=1, keepdims=True) + jnp.sum(high * high, axis=1, keepdims=True)
    scale = lax.rsqrt(total / (2 * half) + epsilon)
    gain = gain_ref[...]
    low = (low * scale * gain[:, :half]).astype(bf16)
    high = (high * scale * gain[:, half:]).astype(bf16)
    product = mm(low, proj_ref[:half, :]) + mm(high, proj_ref[half:, :])
    mid = (residual_ref[...].astype(f32) + product).astype(bf16)
    mid_ref[...] = mid
    rows = mid.shape[0]
    table = slots_of(ids_ref[...], experts, capacity).astype(f32)
    table = table.reshape(experts * capacity, rows).astype(bf16)
    sent_ref[...] = mm(table, mid).astype(bf16)


def expert_kernel(own_ref, other_ref, gain_ref, gate_ref, up_ref, down_ref, keep_ref, send_ref, rows_ref, sum_ref):
    step = pl.program_id(0)
    half = own_ref.shape[1]
    tp = lax.axis_index("tp")

    @pl.when(step == 0)
    def _():
        own, other = own_ref[...].astype(f32), other_ref[...].astype(f32)
        low, high = jnp.where(tp == 0, own, other), jnp.where(tp == 0, other, own)
        total = jnp.sum(low * low, axis=1, keepdims=True) + jnp.sum(
            high * high, axis=1, keepdims=True
        )
        scale = lax.rsqrt(total / (2 * half) + epsilon)
        gain = gain_ref[...]
        rows_ref[:, :half] = (low * scale * gain[:, :half]).astype(bf16)
        rows_ref[:, half:] = (high * scale * gain[:, half:]).astype(bf16)

    rows = rows_ref[...]
    gated = jnp.minimum(mm(rows, gate_ref[...]), clamp_limit)
    lifted = jnp.clip(mm(rows, up_ref[...]), -clamp_limit, clamp_limit) + 1.0
    active = (lifted * gated * jax.nn.sigmoid(swish_alpha * gated)).astype(bf16)
    product = mm(active, down_ref[...])

    @pl.when(step == 0)
    def _():
        sum_ref[...] = product

    @pl.when(step > 0)
    def _():
        sum_ref[...] += product

    @pl.when(step == pl.num_programs(0) - 1)
    def _():
        mine = pl.multiple_of(tp * half, half)
        theirs = pl.multiple_of((1 - tp) * half, half)
        keep_ref[...] = sum_ref[:, pl.ds(mine, half)].astype(bf16)
        send_ref[...] = sum_ref[:, pl.ds(theirs, half)].astype(bf16)


def combine_kernel(capacity, experts, ids_ref, weights_ref, mid_ref, back_ref, out_ref):
    ids = ids_ref[...]
    rows = ids.shape[1]
    mask = slots_of(ids, experts, capacity)
    expert = lax.broadcasted_iota(jnp.int32, (experts, rows), 0)
    weight = jnp.zeros((experts, rows), f32)
    for k in range(ids.shape[0]):
        weight = weight + jnp.where(ids[k : k + 1, :] == expert, weights_ref[k : k + 1, :], 0.0)
    table = jnp.where(mask, weight[:, None, :], 0.0).reshape(experts * capacity, rows)
    high, low = split(table)
    back = back_ref[...]
    total = mm(high, back, TN) + mm(low, back, TN)
    out_ref[...] = (mid_ref[...].astype(f32) + total).astype(bf16)


def local(
    residual,
    route_ids,
    route_weights,
    carried_state,
    mix_gain,
    in_proj,
    decay_rate,
    frequency,
    step_size,
    input_map,
    output_matrix,
    passthrough_scale,
    out_gain,
    out_proj,
    ffn_gain,
    w_gate,
    w_up,
    w_down,
):
    rows, half = residual.shape
    top = route_ids.shape[1]
    peers = lax.axis_size("ep")
    experts = w_gate.shape[0] * peers
    capacity = max(2, 3 * rows * top // (2 * experts))
    capacity = -(-capacity // 8) * 8
    channel_half = in_proj.shape[1]
    hidden = w_gate.shape[2]
    swap = [(0, 1), (1, 0)]
    ids, weights = route_ids.T, route_weights.T
    params = pltpu.CompilerParams(vmem_limit_bytes=48 * 1024 * 1024)

    other = lax.ppermute(residual, "tp", swap)
    active, new_state = pl.pallas_call(
        mixer_kernel,
        out_shape=(
            jax.ShapeDtypeStruct((rows, channel_half), bf16),
            jax.ShapeDtypeStruct(carried_state.shape, f32),
        ),
        compiler_params=params,
        name="mixer",
    )(
        residual,
        other,
        carried_state,
        mix_gain.reshape(1, -1),
        in_proj,
        decay_rate,
        frequency,
        step_size.reshape(1, -1),
        jnp.swapaxes(input_map, 2, 3),
        output_matrix,
        passthrough_scale.reshape(1, -1),
    )
    other = lax.ppermute(active, "tp", swap)
    slots = experts * capacity
    mid, sent = pl.pallas_call(
        functools.partial(dispatch_kernel, capacity, experts),
        out_shape=(
            jax.ShapeDtypeStruct((rows, half), bf16),
            jax.ShapeDtypeStruct((slots, half), bf16),
        ),
        compiler_params=params,
        name="dispatch",
    )(active, other, out_gain.reshape(1, -1), out_proj, residual, ids)

    def exchange(values):
        values = values.reshape(peers, slots // peers, half)
        values = lax.all_to_all(values, "ep", split_axis=0, concat_axis=0, tiled=True)
        return values.reshape(slots, half)

    arrived = exchange(sent)
    other = lax.ppermute(arrived, "tp", swap)
    tiles = max(1, hidden // 256)
    tile = hidden // tiles
    keep, send = pl.pallas_call(
        expert_kernel,
        grid=(tiles,),
        in_specs=[
            pl.BlockSpec((slots, half), lambda j: (0, 0)),
            pl.BlockSpec((slots, half), lambda j: (0, 0)),
            pl.BlockSpec((1, 2 * half), lambda j: (0, 0)),
            pl.BlockSpec((None, 2 * half, tile), lambda j: (0, 0, j)),
            pl.BlockSpec((None, 2 * half, tile), lambda j: (0, 0, j)),
            pl.BlockSpec((None, tile, 2 * half), lambda j: (0, j, 0)),
        ],
        out_specs=(
            pl.BlockSpec((slots, half), lambda j: (0, 0)),
            pl.BlockSpec((slots, half), lambda j: (0, 0)),
        ),
        out_shape=(jax.ShapeDtypeStruct((slots, half), bf16),) * 2,
        scratch_shapes=[pltpu.VMEM((slots, 2 * half), bf16), pltpu.VMEM((slots, 2 * half), f32)],
        compiler_params=params,
        name="experts",
    )(arrived, other, ffn_gain.reshape(1, -1), w_gate, w_up, w_down)
    other = lax.ppermute(send, "tp", swap)
    back = exchange((keep.astype(f32) + other.astype(f32)).astype(bf16))
    updated = pl.pallas_call(
        functools.partial(combine_kernel, capacity, experts),
        out_shape=jax.ShapeDtypeStruct((rows, half), bf16),
        compiler_params=params,
        name="combine",
    )(ids, weights, mid, back)
    return updated, new_state


def solution(mesh):
    placed = (
        P("ep", "tp"),
        P("ep", None),
        P("ep", None),
        P(None, "ep", "tp"),
        P(),
        P(None, "tp"),
        P("tp", None),
        P("tp", None),
        P("tp"),
        P(None, "tp", None, None),
        P(None, "tp", None, None),
        P("tp"),
        P(),
        P(None, "tp"),
        P(),
        P("ep", None, "tp"),
        P("ep", None, "tp"),
        P("ep", "tp", None),
    )
    return jax.shard_map(
        local,
        mesh=mesh,
        in_specs=placed,
        out_specs=(P("ep", "tp"), P(None, "ep", "tp")),
        check_vma=False,
    )
```

```python
import functools

import jax
import jax.numpy as jnp
from jax import lax
from jax.experimental import pallas as pl
from jax.experimental.pallas import tpu as pltpu
from jax.sharding import PartitionSpec as P


epsilon = 1e-06
clamp_limit = 7.0
swish_alpha = 1.702
f32, bf16 = jnp.float32, jnp.bfloat16
NN = (((1,), (0,)), ((), ()))
NT = (((1,), (1,)), ((), ()))
TN = (((0,), (0,)), ((), ()))
MIXER_VMEM = 16
HEAD_FLOPS = 10**11


def mm(a, b, dims=NN):
    return lax.dot_general(a, b, dims, preferred_element_type=f32)


def split(values):
    high = values.astype(bf16)
    return high, (values - high.astype(f32)).astype(bf16)


def flat_row(table):
    groups, width = table.shape
    tiled = jnp.concatenate([table] * groups, axis=1)
    lane = lax.broadcasted_iota(jnp.int32, tiled.shape, 1)
    first = lax.broadcasted_iota(jnp.int32, tiled.shape, 0) * width
    own = (lane >= first) & (lane < first + width)
    return jnp.sum(jnp.where(own, tiled, 0.0), axis=0, keepdims=True)


def spread(table, count):
    _, per_group, width = table.shape
    tiled = jnp.concatenate([table] * count, axis=2)
    lane = lax.broadcasted_iota(jnp.int32, tiled.shape, 2)
    first = lax.broadcasted_iota(jnp.int32, tiled.shape, 0) * width
    own = (lane >= first) & (lane < first + width)
    return jnp.where(own, tiled, 0.0).reshape(count * per_group, count * width)


def head_kernel(out_ref):
    out_ref[...] = jnp.zeros_like(out_ref)


def mixer_kernel(*refs):
    decay_ref, freq_ref, step_ref, map_ref, out_ref, own_ref, other_ref, gain_ref = refs[:8]
    proj_ref, skip_ref, ids_ref, weights_ref, state_ref, _, act_ref, new_ref = refs[8:]
    groups, width = decay_ref.shape
    per_group = map_ref.shape[2]
    step = step_ref[...]
    square = jnp.broadcast_to(step, (groups, groups))
    diagonal = lax.broadcasted_iota(jnp.int32, square.shape, 0) == lax.broadcasted_iota(
        jnp.int32, square.shape, 1
    )
    step = jnp.sum(jnp.where(diagonal, square, 0.0), axis=1, keepdims=True)
    rate, freq = -decay_ref[...], freq_ref[...]
    magnitude = jnp.exp(rate * step)
    phase = freq * step
    bar_real, bar_imag = magnitude * jnp.cos(phase), magnitude * jnp.sin(phase)
    inverse = 1.0 / (rate * rate + freq * freq)
    shifted = bar_real - 1.0
    coef_real = ((shifted * rate + bar_imag * freq) * inverse)[:, None, :]
    coef_imag = ((bar_imag * rate - shifted * freq) * inverse)[:, None, :]
    map_real = coef_real * map_ref[0] - coef_imag * map_ref[1]
    map_imag = coef_real * map_ref[1] + coef_imag * map_ref[0]
    bar_real, bar_imag = flat_row(bar_real), flat_row(bar_imag)
    count = max(1, min(groups, 128 // per_group))
    blocks = [slice(i * count, (i + 1) * count) for i in range(groups // count)]
    tables = [
        split(spread(map_real[held], count))
        + split(spread(map_imag[held], count))
        + (spread(out_ref[0, held], count).astype(bf16), spread(-out_ref[1, held], count).astype(bf16))
        for held in blocks
    ]
    low, high = normed(own_ref[...], other_ref[...], gain_ref[...], lax.axis_index("tp") == 0)
    half = low.shape[1]
    channels = (mm(low, proj_ref[:half, :]) + mm(high, proj_ref[half:, :])).astype(bf16)
    rows = low.shape[0]
    lanes, columns = count * width, count * per_group
    for block, (real_high, real_low, imag_high, imag_low, out_real, out_imag) in enumerate(tables):
        wide = slice(block * lanes, (block + 1) * lanes)
        narrow = slice(block * columns, (block + 1) * columns)
        fed = channels[:, narrow]
        old_real, old_imag = state_ref[0, :, wide], state_ref[1, :, wide]
        turn_real, turn_imag = bar_real[:, wide], bar_imag[:, wide]
        next_real = (
            turn_real * old_real - turn_imag * old_imag + (mm(fed, real_high) + mm(fed, real_low))
        )
        next_imag = (
            turn_real * old_imag + turn_imag * old_real + (mm(fed, imag_high) + mm(fed, imag_low))
        )
        new_ref[0, :, wide] = next_real
        new_ref[1, :, wide] = next_imag
        mixed = mm(next_real.astype(bf16), out_real, NT) + mm(next_imag.astype(bf16), out_imag, NT)
        mixed = mixed + skip_ref[:, narrow] * fed.astype(f32)
        act_ref[:rows, narrow] = jax.nn.gelu(mixed).astype(bf16)
    weights = weights_ref[...]
    w_high = weights.astype(bf16).astype(f32)
    w_mid = (weights - w_high).astype(bf16).astype(f32)
    w_low = weights - w_high - w_mid
    parts = (ids_ref[...].astype(f32), w_high, w_mid, w_low)
    top = weights.shape[0]
    each = act_ref.shape[1] // rows
    lines = -(-4 * top // each)
    tags = [
        jnp.concatenate(
            [jnp.concatenate(parts, axis=0)[i : i + 1, :] for i in range(4 * top)][k * each : (k + 1) * each],
            axis=1,
        )
        for k in range(lines)
    ]
    tags.append(jnp.zeros((act_ref.shape[0] - rows - lines, act_ref.shape[1]), f32))
    act_ref[rows:, :] = jnp.concatenate(tags, axis=0).astype(bf16)


def normed(own, other, gain, first):
    own, other = own.astype(f32), other.astype(f32)
    half = own.shape[1]
    low, high = jnp.where(first, own, other), jnp.where(first, other, own)
    total = jnp.sum(low * low, axis=1, keepdims=True) + jnp.sum(high * high, axis=1, keepdims=True)
    scale = lax.rsqrt(total / (2 * half) + epsilon)
    return (
        (low * scale * gain[:, :half]).astype(bf16),
        (high * scale * gain[:, half:]).astype(bf16),
    )


def dispatch_kernel(
    chosen,
    span,
    top,
    own_ref,
    other_ref,
    far_own_ref,
    far_other_ref,
    gain_ref,
    proj_ref,
    residual_ref,
    far_residual_ref,
    mid_ref,
    high_ref,
    low_ref,
    *sent_refs,
):
    first = lax.axis_index("tp") == 0
    count = residual_ref.shape[0]
    own = jnp.concatenate([own_ref[:count], far_own_ref[:count]], axis=0)
    other = jnp.concatenate([other_ref[:count], far_other_ref[:count]], axis=0)
    low, high = normed(own, other, gain_ref[...], first)
    half = own.shape[1]
    product = mm(low, proj_ref[:half, :]) + mm(high, proj_ref[half:, :])
    residual = jnp.concatenate([residual_ref[...], far_residual_ref[...]], axis=0)
    mid = (residual.astype(f32) + product).astype(bf16)
    mid_ref[...] = mid[: mid_ref.shape[0]]

    each = half // count
    tags = [ref[count:].astype(f32) for ref in (own_ref, far_own_ref)]
    tags = jnp.concatenate(
        [
            jnp.concatenate(
                [
                    tag[i // each : i // each + 1, i % each * count : (i % each + 1) * count]
                    for i in range(4 * top)
                ],
                axis=0,
            )
            for tag in tags
        ],
        axis=1,
    )
    rows = tags.shape[1]
    ids = tags[:top].astype(jnp.int32)
    weights = tags[top : 2 * top] + tags[2 * top : 3 * top] + tags[3 * top :]
    place = lax.axis_index("ep")
    base = place // chosen * chosen
    turn = lax.broadcasted_iota(jnp.int32, (chosen, rows), 0)
    expert = base + (turn ^ (place - base))
    named = jnp.zeros((chosen, rows), f32)
    weight = jnp.zeros((chosen, rows), f32)
    for k in range(top):
        same = ids[k : k + 1, :] == expert
        named = named + same.astype(f32)
        weight = weight + jnp.where(same, weights[k : k + 1, :], 0.0)
    earlier = lax.broadcasted_iota(jnp.int32, (rows, rows), 0) < lax.broadcasted_iota(
        jnp.int32, (rows, rows), 1
    )
    rank = mm(named.astype(bf16), earlier.astype(f32).astype(bf16))
    rank = jnp.where(named > 0.0, rank, -1.0).astype(jnp.int32)
    slot = lax.broadcasted_iota(jnp.int32, (chosen, span, rows), 1)
    mask = rank[:, None, :] == slot
    shape = (chosen * span, rows)
    table = mask.astype(f32).reshape(shape).astype(bf16)
    high_ref[...], low_ref[...] = split(jnp.where(mask, weight[:, None, :], 0.0).reshape(shape))
    sent = mm(table, mid).astype(bf16)
    for t, ref in enumerate(sent_refs):
        ref[...] = sent[t * span : (t + 1) * span]


def pack_kernel(*refs):
    refs[-1][...] = jnp.concatenate([ref[...] for ref in refs[:-1]], axis=0)


def expert_kernel(
    own_ref, other_ref, gain_ref, gate_ref, up_ref, down_ref, keep_ref, send_ref, active_ref
):
    tp = lax.axis_index("tp")
    half = own_ref.shape[1]
    low, high = normed(own_ref[...], other_ref[...], gain_ref[...], tp == 0)
    rows = jnp.concatenate([low, high], axis=1)
    hidden = gate_ref.shape[1]
    tile = min(hidden, 256)
    for j in range(hidden // tile):
        part = slice(j * tile, (j + 1) * tile)
        gated = jnp.minimum(mm(rows, gate_ref[:, part]), clamp_limit)
        lifted = jnp.clip(mm(rows, up_ref[:, part]), -clamp_limit, clamp_limit) + 1.0
        active_ref[:, part] = (lifted * gated * jax.nn.sigmoid(swish_alpha * gated)).astype(bf16)
    active = active_ref[...]
    tile = min(half, 256)
    for ref, start in ((send_ref, (1 - tp) * half), (keep_ref, tp * half)):
        for j in range(half // tile):
            part = pl.ds(pl.multiple_of(start + j * tile, tile), tile)
            ref[:, j * tile : (j + 1) * tile] = mm(active, down_ref[:, part]).astype(bf16)


def add_kernel(keep_ref, other_ref, *out_refs):
    span = out_refs[0].shape[0]
    total = (keep_ref[...].astype(f32) + other_ref[...].astype(f32)).astype(bf16)
    for t, ref in enumerate(out_refs):
        ref[...] = total[t * span : (t + 1) * span]


def combine_kernel(high_ref, low_ref, mid_ref, *refs):
    sum_ref, far_ref = refs[-2:]
    back = jnp.concatenate([ref[...] for ref in refs[:-2]], axis=0)
    total = mm(high_ref[...], back, TN) + mm(low_ref[...], back, TN)
    rows = sum_ref.shape[0]
    far_ref[...] = total[rows:].astype(bf16)
    sum_ref[...] = mid_ref[...].astype(f32) + total[:rows]


def final_kernel(sum_ref, far_ref, out_ref):
    out_ref[...] = (sum_ref[...] + far_ref[...].astype(f32)).astype(bf16)


def call(kernel, outs, flops, vmem=8, **more):
    return pl.pallas_call(
        kernel,
        out_shape=tuple(jax.ShapeDtypeStruct(shape, dtype) for shape, dtype in outs),
        compiler_params=pltpu.CompilerParams(vmem_limit_bytes=vmem * 1024 * 1024),
        cost_estimate=pl.CostEstimate(flops=flops, bytes_accessed=10**6, transcendentals=0),
        **more,
    )


def local(
    residual,
    route_ids,
    route_weights,
    carried_state,
    mix_gain,
    in_proj,
    decay_rate,
    frequency,
    step_size,
    input_map,
    output_matrix,
    passthrough_scale,
    out_gain,
    out_proj,
    ffn_gain,
    w_gate,
    w_up,
    w_down,
):
    rows, half = residual.shape
    top = route_ids.shape[1]
    peers = lax.axis_size("ep")
    experts = w_gate.shape[0] * peers
    capacity = max(2, 3 * rows * top // (2 * experts))
    inner = peers // 2
    span = -(-2 * capacity // 16) * 16
    slots = inner * span
    channel_half = in_proj.shape[1]
    hidden = w_gate.shape[2]
    gate, up, down = w_gate[0], w_up[0], w_down[0]

    def across(values):
        return lax.ppermute(values, "tp", [(0, 1), (1, 0)])

    def opposite(values):
        return lax.ppermute(values, "ep", [(e, e ^ inner) for e in range(peers)])

    def within(values, t):
        return lax.ppermute(values, "ep", [(e, e ^ t) for e in range(peers)])

    other = across(residual)
    far_residual = opposite(residual)
    (head,) = call(head_kernel, [((8, 128), f32)], HEAD_FLOPS)()
    operands = (
        decay_rate,
        frequency,
        step_size.reshape(1, -1),
        jnp.swapaxes(input_map, 2, 3),
        output_matrix,
        residual,
        other,
        mix_gain.reshape(1, -1),
        in_proj,
        passthrough_scale.reshape(1, -1),
        route_ids.T,
        route_weights.T,
        carried_state,
        head,
    )
    active, new_state = call(
        mixer_kernel,
        [((rows + 8, channel_half), bf16), (carried_state.shape, f32)],
        10**9,
        MIXER_VMEM,
    )(*operands)
    far_active = opposite(active)
    mid, high, low, *sent = call(
        functools.partial(dispatch_kernel, inner, span, top),
        [((rows, half), bf16)]
        + [((slots, 2 * rows), bf16)] * 2
        + [((span, half), bf16)] * inner,
        10**10,
    )(
        active,
        across(active),
        far_active,
        across(far_active),
        out_gain.reshape(1, -1),
        out_proj,
        residual,
        far_residual,
    )
    got = {t: within(sent[t], t) for t in range(1, inner)}
    got[0] = sent[0]
    back = []
    for turns in (range(inner // 2), range(inner // 2, inner)):
        share = len(turns) * span
        (packed,) = call(pack_kernel, [((share, half), bf16)], 10**6)(*[got[t] for t in turns])
        keep, send = call(
            expert_kernel,
            [((share, half), bf16)] * 2,
            12 * share * half * hidden,
            scratch_shapes=[pltpu.VMEM((share, hidden), bf16)],
        )(packed, across(packed), ffn_gain.reshape(1, -1), gate, up, down)
        sums = call(add_kernel, [((span, half), bf16)] * len(turns), 10**6)(keep, across(send))
        back += [within(value, t) if t else value for t, value in zip(turns, sums)]
    total, far = call(
        combine_kernel, [((rows, half), f32), ((rows, half), bf16)], 10**8
    )(high, low, mid, *back)
    (updated,) = call(final_kernel, [((rows, half), bf16)], 10**6)(total, opposite(far))
    return updated, new_state


def solution(mesh):
    placed = (
        P("ep", "tp"),
        P("ep", None),
        P("ep", None),
        P(None, "ep", "tp"),
        P(),
        P(None, "tp"),
        P("tp", None),
        P("tp", None),
        P("tp"),
        P(None, "tp", None, None),
        P(None, "tp", None, None),
        P("tp"),
        P(),
        P(None, "tp"),
        P(),
        P("ep", None, "tp"),
        P("ep", None, "tp"),
        P("ep", "tp", None),
    )

    return jax.shard_map(
        local,
        mesh=mesh,
        in_specs=placed,
        out_specs=(P("ep", "tp"), P(None, "ep", "tp")),
        check_vma=False,
    )
```

```python
import functools

import jax
import jax.numpy as jnp
from jax import lax
from jax.experimental import pallas as pl
from jax.experimental.pallas import tpu as pltpu
from jax.sharding import PartitionSpec as P


epsilon = 1e-06
clamp_limit = 7.0
swish_alpha = 1.702
f32, bf16 = jnp.float32, jnp.bfloat16
NN = (((1,), (0,)), ((), ()))
NT = (((1,), (1,)), ((), ()))
TN = (((0,), (0,)), ((), ()))
MIXER_VMEM = 16
HEAD_FLOPS = 10**11


def mm(a, b, dims=NN):
    return lax.dot_general(a, b, dims, preferred_element_type=f32)


def split(values):
    high = values.astype(bf16)
    return high, (values - high.astype(f32)).astype(bf16)


def flat_row(table):
    groups, width = table.shape
    tiled = jnp.concatenate([table] * groups, axis=1)
    lane = lax.broadcasted_iota(jnp.int32, tiled.shape, 1)
    first = lax.broadcasted_iota(jnp.int32, tiled.shape, 0) * width
    own = (lane >= first) & (lane < first + width)
    return jnp.sum(jnp.where(own, tiled, 0.0), axis=0, keepdims=True)


def spread(table, count):
    _, per_group, width = table.shape
    tiled = jnp.concatenate([table] * count, axis=2)
    lane = lax.broadcasted_iota(jnp.int32, tiled.shape, 2)
    first = lax.broadcasted_iota(jnp.int32, tiled.shape, 0) * width
    own = (lane >= first) & (lane < first + width)
    return jnp.where(own, tiled, 0.0).reshape(count * per_group, count * width)


def head_kernel(out_ref):
    out_ref[...] = jnp.zeros_like(out_ref)


def mixer_kernel(*refs):
    decay_ref, freq_ref, step_ref, map_ref, out_ref, own_ref, other_ref, gain_ref = refs[:8]
    proj_ref, skip_ref, ids_ref, weights_ref, state_ref, _, act_ref, new_ref = refs[8:]
    groups, width = decay_ref.shape
    per_group = map_ref.shape[2]
    step = step_ref[...]
    square = jnp.broadcast_to(step, (groups, groups))
    diagonal = lax.broadcasted_iota(jnp.int32, square.shape, 0) == lax.broadcasted_iota(
        jnp.int32, square.shape, 1
    )
    step = jnp.sum(jnp.where(diagonal, square, 0.0), axis=1, keepdims=True)
    rate, freq = -decay_ref[...], freq_ref[...]
    magnitude = jnp.exp(rate * step)
    phase = freq * step
    bar_real, bar_imag = magnitude * jnp.cos(phase), magnitude * jnp.sin(phase)
    inverse = 1.0 / (rate * rate + freq * freq)
    shifted = bar_real - 1.0
    coef_real = ((shifted * rate + bar_imag * freq) * inverse)[:, None, :]
    coef_imag = ((bar_imag * rate - shifted * freq) * inverse)[:, None, :]
    map_real = coef_real * map_ref[0] - coef_imag * map_ref[1]
    map_imag = coef_real * map_ref[1] + coef_imag * map_ref[0]
    bar_real, bar_imag = flat_row(bar_real), flat_row(bar_imag)
    count = max(1, min(groups, 128 // per_group))
    blocks = [slice(i * count, (i + 1) * count) for i in range(groups // count)]
    tables = [
        split(spread(map_real[held], count))
        + split(spread(map_imag[held], count))
        + (spread(out_ref[0, held], count).astype(bf16), spread(-out_ref[1, held], count).astype(bf16))
        for held in blocks
    ]
    low, high = normed(own_ref[...], other_ref[...], gain_ref[...], lax.axis_index("tp") == 0)
    half = low.shape[1]
    channels = (mm(low, proj_ref[:half, :]) + mm(high, proj_ref[half:, :])).astype(bf16)
    rows = low.shape[0]
    lanes, columns = count * width, count * per_group
    for block, (real_high, real_low, imag_high, imag_low, out_real, out_imag) in enumerate(tables):
        wide = slice(block * lanes, (block + 1) * lanes)
        narrow = slice(block * columns, (block + 1) * columns)
        fed = channels[:, narrow]
        old_real, old_imag = state_ref[0, :, wide], state_ref[1, :, wide]
        turn_real, turn_imag = bar_real[:, wide], bar_imag[:, wide]
        next_real = (
            turn_real * old_real - turn_imag * old_imag + (mm(fed, real_high) + mm(fed, real_low))
        )
        next_imag = (
            turn_real * old_imag + turn_imag * old_real + (mm(fed, imag_high) + mm(fed, imag_low))
        )
        new_ref[0, :, wide] = next_real
        new_ref[1, :, wide] = next_imag
        mixed = mm(next_real.astype(bf16), out_real, NT) + mm(next_imag.astype(bf16), out_imag, NT)
        mixed = mixed + skip_ref[:, narrow] * fed.astype(f32)
        act_ref[:rows, narrow] = jax.nn.gelu(mixed).astype(bf16)
    weights = weights_ref[...]
    w_high = weights.astype(bf16).astype(f32)
    w_mid = (weights - w_high).astype(bf16).astype(f32)
    w_low = weights - w_high - w_mid
    parts = (ids_ref[...].astype(f32), w_high, w_mid, w_low)
    top = weights.shape[0]
    each = act_ref.shape[1] // rows
    lines = -(-4 * top // each)
    tags = [
        jnp.concatenate(
            [jnp.concatenate(parts, axis=0)[i : i + 1, :] for i in range(4 * top)][k * each : (k + 1) * each],
            axis=1,
        )
        for k in range(lines)
    ]
    tags.append(jnp.zeros((act_ref.shape[0] - rows - lines, act_ref.shape[1]), f32))
    act_ref[rows:, :] = jnp.concatenate(tags, axis=0).astype(bf16)


def normed(own, other, gain, first):
    own, other = own.astype(f32), other.astype(f32)
    half = own.shape[1]
    low, high = jnp.where(first, own, other), jnp.where(first, other, own)
    total = jnp.sum(low * low, axis=1, keepdims=True) + jnp.sum(high * high, axis=1, keepdims=True)
    scale = lax.rsqrt(total / (2 * half) + epsilon)
    return (
        (low * scale * gain[:, :half]).astype(bf16),
        (high * scale * gain[:, half:]).astype(bf16),
    )


def tables(own_ref, rows, top, chosen, span, turned):
    half = own_ref.shape[1]
    each = half // rows
    tags = own_ref[rows:].astype(f32)
    tags = jnp.concatenate(
        [
            tags[i // each : i // each + 1, i % each * rows : (i % each + 1) * rows]
            for i in range(4 * top)
        ],
        axis=0,
    )
    ids = tags[:top].astype(jnp.int32)
    weights = tags[top : 2 * top] + tags[2 * top : 3 * top] + tags[3 * top :]
    place = lax.axis_index("ep")
    base = place // chosen * chosen
    turn = lax.broadcasted_iota(jnp.int32, (chosen, rows), 0)
    earlier = lax.broadcasted_iota(jnp.int32, (rows, rows), 0) < lax.broadcasted_iota(
        jnp.int32, (rows, rows), 1
    )
    slot = lax.broadcasted_iota(jnp.int32, (chosen, span, rows), 1)

    def masked(expert):
        named = jnp.zeros((chosen, rows), f32)
        weight = jnp.zeros((chosen, rows), f32)
        for k in range(top):
            same = ids[k : k + 1, :] == expert
            named = named + same.astype(f32)
            weight = weight + jnp.where(same, weights[k : k + 1, :], 0.0)
        rank = mm(named.astype(bf16), earlier.astype(f32).astype(bf16))
        rank = jnp.where(named > 0.0, rank, -1.0).astype(jnp.int32)
        return rank[:, None, :] == slot, weight[:, None, :]

    selected, weight = masked(base + (turn ^ (place - base)))
    mask = selected
    if not turned:
        mask, weight = masked(base + turn)
    return selected.astype(f32), jnp.where(mask, weight, 0.0).reshape(chosen * span, rows)


def dispatch_kernel(
    span,
    top,
    own_ref,
    other_ref,
    far_own_ref,
    far_other_ref,
    gain_ref,
    proj_ref,
    residual_ref,
    far_residual_ref,
    mid_ref,
    high_ref,
    low_ref,
    far_high_ref,
    far_low_ref,
    *sent_refs,
):
    rows = residual_ref.shape[0]
    chosen = len(sent_refs)
    own = jnp.concatenate([own_ref[:rows], far_own_ref[:rows]], axis=0)
    other = jnp.concatenate([other_ref[:rows], far_other_ref[:rows]], axis=0)
    low, high = normed(own, other, gain_ref[...], lax.axis_index("tp") == 0)
    half = low.shape[1]
    product = mm(low, proj_ref[:half, :]) + mm(high, proj_ref[half:, :])
    residual = jnp.concatenate([residual_ref[...], far_residual_ref[...]], axis=0)
    mid = (residual.astype(f32) + product).astype(bf16)
    mid_ref[...] = mid[:rows]
    near, near_weights = tables(own_ref, rows, top, chosen, span, True)
    far, far_weights = tables(far_own_ref, rows, top, chosen, span, False)
    high_ref[...], low_ref[...] = split(near_weights)
    far_high_ref[...], far_low_ref[...] = split(far_weights)
    none = jnp.zeros_like(near)
    table = jnp.concatenate(
        [jnp.concatenate([near, none], axis=2), jnp.concatenate([none, far], axis=2)], axis=1
    )
    table = table.reshape(2 * chosen * span, 2 * rows).astype(bf16)
    sent = mm(table, mid)
    for t, ref in enumerate(sent_refs):
        ref[...] = sent[2 * t * span : 2 * (t + 1) * span].astype(bf16)


def pack_kernel(*refs):
    refs[-1][...] = jnp.concatenate([ref[...] for ref in refs[:-1]], axis=0)


def scaled_half(ref, gain_ref, side):
    values = ref[...].astype(f32)
    width = values.shape[1]
    total = jnp.sum(values * values, axis=1, keepdims=True)
    part = pl.ds(pl.multiple_of(side * width, width), width)
    return (values * gain_ref[:, part]).astype(bf16), total, part


def own_kernel(own_ref, gain_ref, gate_ref, up_ref, gate_sum_ref, up_sum_ref, total_ref):
    rows, total, part = scaled_half(own_ref, gain_ref, lax.axis_index("tp"))
    total_ref[...] = jnp.broadcast_to(total, total_ref.shape)
    hidden = gate_ref.shape[1]
    tile = min(hidden, 256)
    for j in range(hidden // tile):
        col = slice(j * tile, (j + 1) * tile)
        gate_sum_ref[:, col] = mm(rows, gate_ref[part, col])
        up_sum_ref[:, col] = mm(rows, up_ref[part, col])


def expert_kernel(
    other_ref,
    gate_sum_ref,
    up_sum_ref,
    total_ref,
    gain_ref,
    gate_ref,
    up_ref,
    down_ref,
    active_ref,
    send_ref,
):
    theirs = 1 - lax.axis_index("tp")
    rows, total, part = scaled_half(other_ref, gain_ref, theirs)
    half = rows.shape[1]
    scale = lax.rsqrt((total + total_ref[:, :1]) / (2 * half) + epsilon)
    hidden = gate_ref.shape[1]
    tile = min(hidden, 256)
    for j in range(hidden // tile):
        col = slice(j * tile, (j + 1) * tile)
        gate = (gate_sum_ref[:, col] + mm(rows, gate_ref[part, col])) * scale
        up = (up_sum_ref[:, col] + mm(rows, up_ref[part, col])) * scale
        gated = jnp.minimum(gate, clamp_limit)
        lifted = jnp.clip(up, -clamp_limit, clamp_limit) + 1.0
        active_ref[:, col] = (lifted * gated * jax.nn.sigmoid(swish_alpha * gated)).astype(bf16)
    lower(active_ref, down_ref, theirs, send_ref)


def lower(active_ref, down_ref, side, out_ref):
    active = active_ref[...]
    half = out_ref.shape[1]
    tile = min(half, 256)
    for j in range(half // tile):
        part = pl.ds(pl.multiple_of(side * half + j * tile, tile), tile)
        out_ref[:, j * tile : (j + 1) * tile] = mm(active, down_ref[:, part]).astype(bf16)


def keep_kernel(active_ref, down_ref, keep_ref):
    lower(active_ref, down_ref, lax.axis_index("tp"), keep_ref)


def add_kernel(*refs):
    refs, far_ref, near_refs = refs[:4], refs[4], refs[5:]
    chosen, span, _ = far_ref.shape
    place = lax.axis_index("ep") % chosen
    first = 0
    for keep_ref, other_ref in zip(refs[::2], refs[1::2]):
        total = keep_ref[...].astype(f32) + other_ref[...].astype(f32)
        for i in range(total.shape[0] // (2 * span)):
            member = (first + i) ^ place
            near_refs[first + i][...] = total[2 * i * span : (2 * i + 1) * span].astype(bf16)
            far_ref[member] = total[(2 * i + 1) * span : 2 * (i + 1) * span].astype(bf16)
        first += total.shape[0] // (2 * span)


def weighted(high_ref, low_ref, refs):
    back = jnp.concatenate([ref[...].astype(f32) for ref in refs], axis=0).astype(bf16)
    return mm(high_ref[...], back, TN) + mm(low_ref[...], back, TN)


def combine_kernel(high_ref, low_ref, back_ref, out_ref):
    out_ref[...] = weighted(high_ref, low_ref, (back_ref,)).astype(bf16)


def final_kernel(high_ref, low_ref, mid_ref, far_ref, *refs):
    total = mid_ref[...].astype(f32) + far_ref[...].astype(f32)
    refs[-1][...] = (total + weighted(high_ref, low_ref, refs[:-1])).astype(bf16)


def call(kernel, outs, flops, vmem=8, **more):
    return pl.pallas_call(
        kernel,
        out_shape=tuple(jax.ShapeDtypeStruct(shape, dtype) for shape, dtype in outs),
        compiler_params=pltpu.CompilerParams(vmem_limit_bytes=vmem * 1024 * 1024),
        cost_estimate=pl.CostEstimate(flops=flops, bytes_accessed=10**6, transcendentals=0),
        **more,
    )


def local(
    residual,
    route_ids,
    route_weights,
    carried_state,
    mix_gain,
    in_proj,
    decay_rate,
    frequency,
    step_size,
    input_map,
    output_matrix,
    passthrough_scale,
    out_gain,
    out_proj,
    ffn_gain,
    w_gate,
    w_up,
    w_down,
):
    rows, half = residual.shape
    top = route_ids.shape[1]
    peers = lax.axis_size("ep")
    experts = w_gate.shape[0] * peers
    capacity = max(2, 3 * rows * top // (2 * experts))
    inner = peers // 2
    span = -(-capacity // 8) * 8
    slots = inner * span
    channel_half = in_proj.shape[1]
    hidden = w_gate.shape[2]
    gate, up, down = w_gate[0], w_up[0], w_down[0]

    def across(values):
        return lax.ppermute(values, "tp", [(0, 1), (1, 0)])

    def opposite(values):
        return lax.ppermute(values, "ep", [(e, e ^ inner) for e in range(peers)])

    def within(values, t):
        return lax.ppermute(values, "ep", [(e, e ^ t) for e in range(peers)])

    cubes = [[h * inner + i for i in range(inner)] for h in range(2)]

    def returned(values):
        values = lax.all_to_all(
            values, "ep", split_axis=0, concat_axis=0, tiled=True, axis_index_groups=cubes
        )
        return values.reshape(slots, half)

    other = across(residual)
    far_residual = opposite(residual)
    (head,) = call(head_kernel, [((8, 128), f32)], HEAD_FLOPS)()
    operands = (
        decay_rate,
        frequency,
        step_size.reshape(1, -1),
        jnp.swapaxes(input_map, 2, 3),
        output_matrix,
        residual,
        other,
        mix_gain.reshape(1, -1),
        in_proj,
        passthrough_scale.reshape(1, -1),
        route_ids.T,
        route_weights.T,
        carried_state,
        head,
    )
    active, new_state = call(
        mixer_kernel,
        [((rows + 8, channel_half), bf16), (carried_state.shape, f32)],
        10**9,
        MIXER_VMEM,
    )(*operands)
    far_active = opposite(active)
    mid, high, low, far_high, far_low, *sent = call(
        functools.partial(dispatch_kernel, span, top),
        [((rows, half), bf16)]
        + [((slots, rows), bf16)] * 4
        + [((2 * span, half), bf16)] * inner,
        10**10,
    )(
        active,
        across(active),
        far_active,
        across(far_active),
        out_gain.reshape(1, -1),
        out_proj,
        residual,
        far_residual,
    )
    got = {t: within(sent[t], t) for t in range(1, inner)}
    got[0] = sent[0]
    parts = []
    for turns in (range(inner // 2), range(inner // 2, inner)):
        share = 2 * len(turns) * span
        (packed,) = call(pack_kernel, [((share, half), bf16)], 10**6)(*[got[t] for t in turns])
        gain = ffn_gain.reshape(1, -1)
        partial = call(
            own_kernel,
            [((share, hidden), f32)] * 2 + [((share, 128), f32)],
            4 * share * half * hidden,
        )(packed, gain, gate, up)
        state, send = call(
            expert_kernel,
            [((share, hidden), bf16), ((share, half), bf16)],
            6 * share * half * hidden,
        )(across(packed), *partial, gain, gate, up, down)
        (keep,) = call(keep_kernel, [((share, half), bf16)], 2 * share * half * hidden)(state, down)
        parts += [keep, across(send)]
    far, *near = call(
        add_kernel, [((inner, span, half), bf16)] + [((span, half), bf16)] * inner, 10**6
    )(*parts)
    far = returned(far)
    near = [within(near[t], t) if t else near[t] for t in range(inner)]
    (sums,) = call(combine_kernel, [((rows, half), bf16)], 10**8)(
        far_high, far_low, far
    )
    (updated,) = call(final_kernel, [((rows, half), bf16)], 10**6)(
        high, low, mid, opposite(sums), *near
    )
    return updated, new_state


def solution(mesh):
    placed = (
        P("ep", "tp"),
        P("ep", None),
        P("ep", None),
        P(None, "ep", "tp"),
        P(),
        P(None, "tp"),
        P("tp", None),
        P("tp", None),
        P("tp"),
        P(None, "tp", None, None),
        P(None, "tp", None, None),
        P("tp"),
        P(),
        P(None, "tp"),
        P(),
        P("ep", None, "tp"),
        P("ep", None, "tp"),
        P("ep", "tp", None),
    )

    return jax.shard_map(
        local,
        mesh=mesh,
        in_specs=placed,
        out_specs=(P("ep", "tp"), P(None, "ep", "tp")),
        check_vma=False,
    )
```

```python
import functools

import jax
import jax.numpy as jnp
from jax import lax
from jax.experimental import pallas as pl
from jax.experimental.pallas import tpu as pltpu
from jax.sharding import PartitionSpec as P


epsilon = 1e-06
clamp_limit = 7.0
swish_alpha = 1.702
f32, bf16 = jnp.float32, jnp.bfloat16
NN = (((1,), (0,)), ((), ()))
NT = (((1,), (1,)), ((), ()))
TN = (((0,), (0,)), ((), ()))
MIXER_VMEM = 16
HEAD_FLOPS = 10**11
PREPARE_VMEM = 12


def mm(a, b, dims=NN):
    return lax.dot_general(a, b, dims, preferred_element_type=f32)


def split(values):
    high = values.astype(bf16)
    return high, (values - high.astype(f32)).astype(bf16)


def flat_row(table):
    groups, width = table.shape
    tiled = jnp.concatenate([table] * groups, axis=1)
    lane = lax.broadcasted_iota(jnp.int32, tiled.shape, 1)
    first = lax.broadcasted_iota(jnp.int32, tiled.shape, 0) * width
    own = (lane >= first) & (lane < first + width)
    return jnp.sum(jnp.where(own, tiled, 0.0), axis=0, keepdims=True)


def spread(table, count):
    _, per_group, width = table.shape
    tiled = jnp.concatenate([table] * count, axis=2)
    lane = lax.broadcasted_iota(jnp.int32, tiled.shape, 2)
    first = lax.broadcasted_iota(jnp.int32, tiled.shape, 0) * width
    own = (lane >= first) & (lane < first + width)
    return jnp.where(own, tiled, 0.0).reshape(count * per_group, count * width)


def head_kernel(out_ref):
    out_ref[...] = jnp.zeros_like(out_ref)


def prepare_kernel(
    decay_ref, freq_ref, step_ref, map_ref, out_ref, _, bars_ref, tables_ref
):
    groups, _ = decay_ref.shape
    per_group = map_ref.shape[2]
    step = step_ref[...]
    square = jnp.broadcast_to(step, (groups, groups))
    diagonal = lax.broadcasted_iota(jnp.int32, square.shape, 0) == lax.broadcasted_iota(
        jnp.int32, square.shape, 1
    )
    step = jnp.sum(jnp.where(diagonal, square, 0.0), axis=1, keepdims=True)
    rate, freq = -decay_ref[...], freq_ref[...]
    magnitude = jnp.exp(rate * step)
    phase = freq * step
    bar_real, bar_imag = magnitude * jnp.cos(phase), magnitude * jnp.sin(phase)
    inverse = 1.0 / (rate * rate + freq * freq)
    shifted = bar_real - 1.0
    coef_real = ((shifted * rate + bar_imag * freq) * inverse)[:, None, :]
    coef_imag = ((bar_imag * rate - shifted * freq) * inverse)[:, None, :]
    map_real = coef_real * map_ref[0] - coef_imag * map_ref[1]
    map_imag = coef_real * map_ref[1] + coef_imag * map_ref[0]
    bars_ref[...] = jnp.concatenate([flat_row(bar_real), flat_row(bar_imag)], axis=0)
    count = tables_ref.shape[2] // per_group
    for i in range(groups // count):
        held = slice(i * count, (i + 1) * count)
        parts = split(spread(map_real[held], count)) + split(spread(map_imag[held], count))
        for k, part in enumerate(parts):
            tables_ref[i, k] = part
        tables_ref[i, 4] = spread(out_ref[0, held], count).astype(bf16)
        tables_ref[i, 5] = spread(-out_ref[1, held], count).astype(bf16)


def mixer_kernel(*refs):
    bars_ref, tables_ref, own_ref, other_ref, gain_ref, proj_ref, skip_ref = refs[:7]
    ids_ref, weights_ref, state_ref, act_ref, new_ref = refs[7:]
    low, high = normed(own_ref[...], other_ref[...], gain_ref[...], lax.axis_index("tp") == 0)
    half = low.shape[1]
    channels = (mm(low, proj_ref[:half, :]) + mm(high, proj_ref[half:, :])).astype(bf16)
    rows = low.shape[0]
    blocks, _, columns, lanes = tables_ref.shape
    for block in range(blocks):
        real_high, real_low, imag_high, imag_low, out_real, out_imag = (
            tables_ref[block, k] for k in range(6)
        )
        wide = slice(block * lanes, (block + 1) * lanes)
        narrow = slice(block * columns, (block + 1) * columns)
        fed = channels[:, narrow]
        old_real, old_imag = state_ref[0, :, wide], state_ref[1, :, wide]
        turn_real, turn_imag = bars_ref[:1, wide], bars_ref[1:, wide]
        next_real = (
            turn_real * old_real - turn_imag * old_imag + (mm(fed, real_high) + mm(fed, real_low))
        )
        next_imag = (
            turn_real * old_imag + turn_imag * old_real + (mm(fed, imag_high) + mm(fed, imag_low))
        )
        new_ref[0, :, wide] = next_real
        new_ref[1, :, wide] = next_imag
        mixed = mm(next_real.astype(bf16), out_real, NT) + mm(next_imag.astype(bf16), out_imag, NT)
        mixed = mixed + skip_ref[:, narrow] * fed.astype(f32)
        act_ref[:rows, narrow] = jax.nn.gelu(mixed).astype(bf16)
    weights = weights_ref[...]
    w_high = weights.astype(bf16).astype(f32)
    w_mid = (weights - w_high).astype(bf16).astype(f32)
    w_low = weights - w_high - w_mid
    parts = (ids_ref[...].astype(f32), w_high, w_mid, w_low)
    top = weights.shape[0]
    each = act_ref.shape[1] // rows
    lines = -(-4 * top // each)
    tags = [
        jnp.concatenate(
            [jnp.concatenate(parts, axis=0)[i : i + 1, :] for i in range(4 * top)][k * each : (k + 1) * each],
            axis=1,
        )
        for k in range(lines)
    ]
    tags.append(jnp.zeros((act_ref.shape[0] - rows - lines, act_ref.shape[1]), f32))
    act_ref[rows:, :] = jnp.concatenate(tags, axis=0).astype(bf16)


def normed(own, other, gain, first):
    own, other = own.astype(f32), other.astype(f32)
    half = own.shape[1]
    low, high = jnp.where(first, own, other), jnp.where(first, other, own)
    total = jnp.sum(low * low, axis=1, keepdims=True) + jnp.sum(high * high, axis=1, keepdims=True)
    scale = lax.rsqrt(total / (2 * half) + epsilon)
    return (
        (low * scale * gain[:, :half]).astype(bf16),
        (high * scale * gain[:, half:]).astype(bf16),
    )


def tables(own_ref, rows, top, chosen, span, turned):
    half = own_ref.shape[1]
    each = half // rows
    tags = own_ref[rows:].astype(f32)
    tags = jnp.concatenate(
        [
            tags[i // each : i // each + 1, i % each * rows : (i % each + 1) * rows]
            for i in range(4 * top)
        ],
        axis=0,
    )
    ids = tags[:top].astype(jnp.int32)
    weights = tags[top : 2 * top] + tags[2 * top : 3 * top] + tags[3 * top :]
    place = lax.axis_index("ep")
    base = place // chosen * chosen
    turn = lax.broadcasted_iota(jnp.int32, (chosen, rows), 0)
    earlier = lax.broadcasted_iota(jnp.int32, (rows, rows), 0) < lax.broadcasted_iota(
        jnp.int32, (rows, rows), 1
    )
    slot = lax.broadcasted_iota(jnp.int32, (chosen, span, rows), 1)

    def masked(expert):
        named = jnp.zeros((chosen, rows), f32)
        weight = jnp.zeros((chosen, rows), f32)
        for k in range(top):
            same = ids[k : k + 1, :] == expert
            named = named + same.astype(f32)
            weight = weight + jnp.where(same, weights[k : k + 1, :], 0.0)
        rank = mm(named.astype(bf16), earlier.astype(f32).astype(bf16))
        rank = jnp.where(named > 0.0, rank, -1.0).astype(jnp.int32)
        return rank[:, None, :] == slot, weight[:, None, :]

    selected, weight = masked(base + (turn ^ (place - base)))
    mask = selected
    if not turned:
        mask, weight = masked(base + turn)
    return selected.astype(f32), jnp.where(mask, weight, 0.0).reshape(chosen * span, rows)


def dispatch_kernel(
    span,
    top,
    own_ref,
    other_ref,
    far_own_ref,
    far_other_ref,
    gain_ref,
    proj_ref,
    residual_ref,
    far_residual_ref,
    mid_ref,
    high_ref,
    low_ref,
    far_high_ref,
    far_low_ref,
    *sent_refs,
):
    rows = residual_ref.shape[0]
    chosen = len(sent_refs)
    own = jnp.concatenate([own_ref[:rows], far_own_ref[:rows]], axis=0)
    other = jnp.concatenate([other_ref[:rows], far_other_ref[:rows]], axis=0)
    low, high = normed(own, other, gain_ref[...], lax.axis_index("tp") == 0)
    half = low.shape[1]
    product = mm(low, proj_ref[:half, :]) + mm(high, proj_ref[half:, :])
    residual = jnp.concatenate([residual_ref[...], far_residual_ref[...]], axis=0)
    mid = (residual.astype(f32) + product).astype(bf16)
    mid_ref[...] = mid[:rows]
    near, near_weights = tables(own_ref, rows, top, chosen, span, True)
    far, far_weights = tables(far_own_ref, rows, top, chosen, span, False)
    high_ref[...], low_ref[...] = split(near_weights)
    far_high_ref[...], far_low_ref[...] = split(far_weights)
    none = jnp.zeros_like(near)
    table = jnp.concatenate(
        [jnp.concatenate([near, none], axis=2), jnp.concatenate([none, far], axis=2)], axis=1
    )
    table = table.reshape(2 * chosen * span, 2 * rows).astype(bf16)
    sent = mm(table, mid)
    for t, ref in enumerate(sent_refs):
        ref[...] = sent[2 * t * span : 2 * (t + 1) * span].astype(bf16)


def store_kernel(value_ref, out_ref):
    out_ref[...] = value_ref[...]


def pack_kernel(*refs):
    refs[-1][...] = jnp.concatenate([ref[...] for ref in refs[:-1]], axis=0)


def scaled_half(ref, gain_ref, side):
    values = ref[...].astype(f32)
    width = values.shape[1]
    total = jnp.sum(values * values, axis=1, keepdims=True)
    part = pl.ds(pl.multiple_of(side * width, width), width)
    return (values * gain_ref[:, part]).astype(bf16), total, part


def own_kernel(own_ref, gain_ref, gate_ref, up_ref, _, gate_sum_ref, up_sum_ref, total_ref):
    rows, total, part = scaled_half(own_ref, gain_ref, lax.axis_index("tp"))
    total_ref[...] = jnp.broadcast_to(total, total_ref.shape)
    hidden = gate_ref.shape[1]
    tile = min(hidden, 256)
    for j in range(hidden // tile):
        col = slice(j * tile, (j + 1) * tile)
        gate_sum_ref[:, col] = mm(rows, gate_ref[part, col])
        up_sum_ref[:, col] = mm(rows, up_ref[part, col])


def expert_kernel(
    other_ref,
    gate_sum_ref,
    up_sum_ref,
    total_ref,
    gain_ref,
    gate_ref,
    up_ref,
    down_ref,
    active_ref,
    send_ref,
):
    theirs = 1 - lax.axis_index("tp")
    rows, total, part = scaled_half(other_ref, gain_ref, theirs)
    half = rows.shape[1]
    scale = lax.rsqrt((total + total_ref[:, :1]) / (2 * half) + epsilon)
    hidden = gate_ref.shape[1]
    tile = min(hidden, 256)
    for j in range(hidden // tile):
        col = slice(j * tile, (j + 1) * tile)
        gate = (gate_sum_ref[:, col] + mm(rows, gate_ref[part, col])) * scale
        up = (up_sum_ref[:, col] + mm(rows, up_ref[part, col])) * scale
        gated = jnp.minimum(gate, clamp_limit)
        lifted = jnp.clip(up, -clamp_limit, clamp_limit) + 1.0
        active_ref[:, col] = (lifted * gated * jax.nn.sigmoid(swish_alpha * gated)).astype(bf16)
    lower(active_ref, down_ref, theirs, send_ref)


def lower(active_ref, down_ref, side, out_ref):
    active = active_ref[...]
    half = out_ref.shape[1]
    tile = min(half, 256)
    for j in range(half // tile):
        part = pl.ds(pl.multiple_of(side * half + j * tile, tile), tile)
        out_ref[:, j * tile : (j + 1) * tile] = mm(active, down_ref[:, part]).astype(bf16)


def keep_kernel(active_ref, down_ref, keep_ref):
    lower(active_ref, down_ref, lax.axis_index("tp"), keep_ref)


def add_kernel(*refs):
    refs, far_ref, near_refs = refs[:4], refs[4], refs[5:]
    chosen, span, _ = far_ref.shape
    place = lax.axis_index("ep") % chosen
    first = 0
    for keep_ref, other_ref in zip(refs[::2], refs[1::2]):
        total = keep_ref[...].astype(f32) + other_ref[...].astype(f32)
        for i in range(total.shape[0] // (2 * span)):
            member = (first + i) ^ place
            near_refs[first + i][...] = total[2 * i * span : (2 * i + 1) * span].astype(bf16)
            far_ref[member] = total[(2 * i + 1) * span : 2 * (i + 1) * span].astype(bf16)
        first += total.shape[0] // (2 * span)


def weighted(high_ref, low_ref, refs):
    back = jnp.concatenate([ref[...].astype(f32) for ref in refs], axis=0).astype(bf16)
    return mm(high_ref[...], back, TN) + mm(low_ref[...], back, TN)


def combine_kernel(high_ref, low_ref, back_ref, out_ref):
    out_ref[...] = weighted(high_ref, low_ref, (back_ref,)).astype(bf16)


def final_kernel(high_ref, low_ref, mid_ref, far_ref, *refs):
    total = mid_ref[...].astype(f32) + far_ref[...].astype(f32)
    refs[-1][...] = (total + weighted(high_ref, low_ref, refs[:-1])).astype(bf16)


def call(kernel, outs, flops, vmem=8, **more):
    return pl.pallas_call(
        kernel,
        out_shape=tuple(jax.ShapeDtypeStruct(shape, dtype) for shape, dtype in outs),
        compiler_params=pltpu.CompilerParams(vmem_limit_bytes=vmem * 1024 * 1024),
        cost_estimate=pl.CostEstimate(flops=flops, bytes_accessed=10**6, transcendentals=0),
        **more,
    )


def local(
    residual,
    route_ids,
    route_weights,
    carried_state,
    mix_gain,
    in_proj,
    decay_rate,
    frequency,
    step_size,
    input_map,
    output_matrix,
    passthrough_scale,
    out_gain,
    out_proj,
    ffn_gain,
    w_gate,
    w_up,
    w_down,
):
    rows, half = residual.shape
    top = route_ids.shape[1]
    peers = lax.axis_size("ep")
    experts = w_gate.shape[0] * peers
    capacity = max(2, 3 * rows * top // (2 * experts))
    inner = peers // 2
    span = -(-capacity // 8) * 8
    slots = inner * span
    channel_half = in_proj.shape[1]
    hidden = w_gate.shape[2]
    gate, up, down = w_gate[0], w_up[0], w_down[0]

    def across(values):
        return lax.ppermute(values, "tp", [(0, 1), (1, 0)])

    def opposite(values):
        return lax.ppermute(values, "ep", [(e, e ^ inner) for e in range(peers)])

    def within(values, t):
        return lax.ppermute(values, "ep", [(e, e ^ t) for e in range(peers)])

    cubes = [[h * inner + i for i in range(inner)] for h in range(2)]

    def returned(values):
        values = lax.all_to_all(
            values, "ep", split_axis=0, concat_axis=0, tiled=True, axis_index_groups=cubes
        )
        return values.reshape(slots, half)

    other = across(residual)
    far_residual = opposite(residual)
    (head,) = call(head_kernel, [((8, 128), f32)], HEAD_FLOPS)()
    groups, width = decay_rate.shape
    per_group = input_map.shape[3]
    count = max(1, min(groups, 128 // per_group))
    bars, tables = call(
        prepare_kernel,
        [
            ((2, groups * width), f32),
            ((groups // count, 6, count * per_group, count * width), bf16),
        ],
        10**6,
        PREPARE_VMEM,
    )(
        decay_rate,
        frequency,
        step_size.reshape(1, -1),
        jnp.swapaxes(input_map, 2, 3),
        output_matrix,
        head,
    )
    operands = (
        bars,
        tables,
        residual,
        other,
        mix_gain.reshape(1, -1),
        in_proj,
        passthrough_scale.reshape(1, -1),
        route_ids.T,
        route_weights.T,
        carried_state,
    )
    active, new_state = call(
        mixer_kernel,
        [((rows + 8, channel_half), bf16), (carried_state.shape, f32)],
        10**9,
        MIXER_VMEM,
    )(*operands)
    far_active = opposite(active)
    (new_state,) = call(store_kernel, [(new_state.shape, f32)], 10**6)(new_state)
    mid, high, low, far_high, far_low, *sent = call(
        functools.partial(dispatch_kernel, span, top),
        [((rows, half), bf16)]
        + [((slots, rows), bf16)] * 4
        + [((2 * span, half), bf16)] * inner,
        10**10,
    )(
        active,
        across(active),
        far_active,
        across(far_active),
        out_gain.reshape(1, -1),
        out_proj,
        residual,
        far_residual,
    )
    got = {t: within(sent[t], t) for t in range(1, inner)}
    got[0] = sent[0]
    parts = []
    for turns in (range(inner // 2), range(inner // 2, inner)):
        share = 2 * len(turns) * span
        (packed,) = call(pack_kernel, [((share, half), bf16)], 10**6)(*[got[t] for t in turns])
        gain = ffn_gain.reshape(1, -1)
        partial = call(
            own_kernel,
            [((share, hidden), f32)] * 2 + [((share, 128), f32)],
            4 * share * half * hidden,
        )(packed, gain, gate, up, down)
        state, send = call(
            expert_kernel,
            [((share, hidden), bf16), ((share, half), bf16)],
            6 * share * half * hidden,
        )(across(packed), *partial, gain, gate, up, down)
        (keep,) = call(keep_kernel, [((share, half), bf16)], 2 * share * half * hidden)(state, down)
        parts += [keep, across(send)]
    far, *near = call(
        add_kernel, [((inner, span, half), bf16)] + [((span, half), bf16)] * inner, 10**6
    )(*parts)
    far = returned(far)
    near = [within(near[t], t) if t else near[t] for t in range(inner)]
    (sums,) = call(combine_kernel, [((rows, half), bf16)], 10**8)(
        far_high, far_low, far
    )
    (updated,) = call(final_kernel, [((rows, half), bf16)], 10**6)(
        high, low, mid, opposite(sums), *near
    )
    return updated, new_state


def solution(mesh):
    placed = (
        P("ep", "tp"),
        P("ep", None),
        P("ep", None),
        P(None, "ep", "tp"),
        P(),
        P(None, "tp"),
        P("tp", None),
        P("tp", None),
        P("tp"),
        P(None, "tp", None, None),
        P(None, "tp", None, None),
        P("tp"),
        P(),
        P(None, "tp"),
        P(),
        P("ep", None, "tp"),
        P("ep", None, "tp"),
        P("ep", "tp", None),
    )

    return jax.shard_map(
        local,
        mesh=mesh,
        in_specs=placed,
        out_specs=(P("ep", "tp"), P(None, "ep", "tp")),
        check_vma=False,
    )
```
